32 devices in a mesh: kv: 4 (over y, x), tp: 8 (over z, core).
Axes of the slice: x: 2, y: 2, z: 4, core: 2. Of those that a mesh axis runs over, the one named last changes fastest.
Arguments:
- tokens: bfloat16 [256, 4096], P('tp', 'kv'), may hold values from -19 to 19, as said below
- lengths: int32 [256], P('kv'), may hold values from 1 to 16384, 1048576 in all
- state_block: float32 [256, 64, 2048], P('kv', None, 'tp'), may hold values from -6 to 6
- cached_keys: bfloat16 [256, 128, 2048], P('kv', None, 'tp'), may hold values from -0.75 to 0.75
- cached_values: bfloat16 [256, 128, 2048], P('kv', None, 'tp'), may hold values from -6 to 6
- query_weight: bfloat16 [4096, 2048], P('kv', 'tp'), may hold values from -0.09375 to 0.09375
- key_weight: bfloat16 [4096, 2048], P('kv', 'tp'), may hold values from -0.09375 to 0.09375
- value_weight: bfloat16 [4096, 2048], P('kv', 'tp'), may hold values from -0.09375 to 0.09375
- gate_weight: bfloat16 [4096, 2048], P('kv', 'tp'), may hold values from -0.09375 to 0.09375
- decay_rate: float32 [32], P('tp'), may hold values from 0.0005 to 0.05
- head_gain: float32 [2048], P('tp'), may hold values from 0.1 to 1.9
- out_weight: bfloat16 [2048, 4096], P('tp', 'kv'), may hold values from -0.125 to 0.125
- mixer_gain: float32 [4096], P('kv'), may hold values from 0.1 to 1.9
- up_weight: bfloat16 [4096, 16384], P('kv', 'tp'), may hold values from -0.09375 to 0.09375
- down_weight: bfloat16 [16384, 4096], P('tp', 'kv'), may hold values from -0.046875 to 0.046875
- final_gain: float32 [4096], P('kv'), may hold values from 0.1 to 1.9
Outputs:
- next_rows: bfloat16 [256, 4096], P('tp', 'kv')
The draws below stay inside these ranges and needn't reach their ends.
Inputs may be any that keep to these rules, and one draw needn't show every extreme that they name: `tokens`: the rows' column groups have scales that differ between groups.
All inputs are finite; a program needn't handle non-finite values. No bound on the sum of `lengths` on one device may be relied on, other than what follows from the above.
Results may differ from the reference program's by a relative error of at most 0.0095.
Values may be sent and summed in bfloat16 or wider, within the bound.
A program may use at most 128 MiB of HBM per device.

```python
import math
import jax
import jax.numpy as jnp
import numpy as np
from jax import lax

D = 4096
HEADS = 32
HDIM = 64
FF = 16384
SEQ_DEV = 64
BLK = 128
LEN_MOST = 16384
RW = 2048
ROWS = 256
LEN_TOTAL = 1048576


def draw_tokens(key, part):
    base, group_key = jax.random.split(jax.random.fold_in(key, 11))
    groups = max(D // 256, 1)
    scales = jnp.exp(jax.random.uniform(group_key, (groups,), jnp.float32, -1.1, 1.1))
    column = jnp.repeat(scales, D // groups, total_repeat_length=D)
    values = jnp.clip(jax.random.normal(base, (ROWS, D), jnp.float32), -6.0, 6.0)
    return (values * column[None, :]).astype(jnp.bfloat16)


def levels(stream_key, dims, cuts, smallest, top_value):
    level, own = 1.0, jax.random.fold_in(stream_key, 6)
    for dim, shards_of in cuts:
        heights = jnp.exp(jax.random.uniform(jax.random.fold_in(own, dim), (shards_of,), jnp.float32, smallest / len(cuts), top_value / len(cuts)))
        level = level * jnp.repeat(heights, dims[dim] // shards_of).reshape([-1 if axis == dim else 1 for axis in range(len(dims))])
    return level


def profile(number_of, total, most, lean):
    weights = [(1 << 20) // math.isqrt(rank ** lean) + 1 for rank in range(2, number_of + 1)]
    spare, counts = total - most - (number_of - 1), [1] * (number_of - 1)
    while spare > 0:
        candidates = [i for i in range(number_of - 1) if counts[i] < most]
        mass, remaining = sum([weights[i] for i in candidates]), spare
        for i in candidates:
            extra = min(most - counts[i], max(1, remaining * weights[i] // mass), spare)
            counts[i] = counts[i] + extra
            spare = spare - extra
    return np.array([most] + counts)


def ragged(key, number_of, total, bound, skew):
    if number_of == 2:
        one = jax.random.randint(key, (), max(1, total - bound), min(bound, total - 1) + 1)
        return jnp.stack([one, total - one])
    tallies = jnp.asarray(profile(number_of, total, bound, skew), jnp.int32)
    pairs = (number_of - 1) // 2
    giver, receiver = tallies[1:1 + 2 * pairs:2], tallies[2:2 + 2 * pairs:2]
    slack = jnp.minimum(giver - 1, bound - receiver)
    passed = jax.random.randint(jax.random.fold_in(key, 1), (pairs,), 0, 1 << 20) % (slack + 1)
    tallies = tallies.at[1:1 + 2 * pairs:2].set(giver - passed).at[2:2 + 2 * pairs:2].set(receiver + passed)
    return tallies[jax.random.permutation(jax.random.fold_in(key, 2), number_of)]


def bell_draw(rng, shape, scale, bound, cuts=(), kind=jnp.bfloat16):
    level = levels(rng, shape, cuts, -0.22, 0.18) if cuts else 1.0
    entries = jax.random.normal(rng, shape, jnp.float32) * scale * level
    return jnp.minimum(jnp.maximum(entries, -bound), bound).astype(kind)


def setup_inputs(seed: int = 0) -> dict:
    seeds = jax.random.split(jax.random.key(seed), 17)
    tokens = draw_tokens(jax.random.fold_in(seeds[16], 71), 0)
    lengths = ragged(seeds[1], ROWS, LEN_TOTAL, LEN_MOST, 2).astype(jnp.int32)
    state_block = bell_draw(seeds[2], (ROWS, HDIM, RW), 1.0, 6.0, ((0, 4), (2, 8)), jnp.float32)
    cached_keys = bell_draw(seeds[3], (ROWS, BLK, RW), 0.125, 0.75, ((0, 4), (2, 8)))
    cached_values = bell_draw(seeds[4], (ROWS, BLK, RW), 1.0, 6.0, ((0, 4), (2, 8)))
    query_weight = bell_draw(seeds[5], (D, RW), D ** -0.5, 0.09375, ((0, 4), (1, 8)))
    key_weight = bell_draw(seeds[6], (D, RW), D ** -0.5, 0.09375, ((0, 4), (1, 8)))
    value_weight = bell_draw(seeds[7], (D, RW), D ** -0.5, 0.09375, ((0, 4), (1, 8)))
    gate_weight = bell_draw(seeds[8], (D, RW), D ** -0.5, 0.09375, ((0, 4), (1, 8)))
    decay_rate = jnp.clip(jnp.exp(math.log(0.05) - 4.6051702 * jax.random.uniform(seeds[9], (HEADS,), jnp.float32) ** levels(seeds[9], (HEADS,), ((0, 8),), -0.2, 0.2)), 0.0005, 0.05)
    head_gain = jnp.clip(1.0 + 0.18 * jax.random.normal(seeds[10], (RW,), jnp.float32), 0.1, 1.9)
    out_weight = bell_draw(seeds[11], (RW, D), RW ** -0.5, 0.125, ((0, 8), (1, 4)))
    mixer_gain = jnp.clip(1.0 + 0.18 * jax.random.normal(seeds[12], (D,), jnp.float32), 0.1, 1.9)
    up_weight = bell_draw(seeds[13], (D, FF), D ** -0.5, 0.09375, ((0, 4), (1, 8)))
    down_weight = bell_draw(seeds[14], (FF, D), FF ** -0.5, 0.046875, ((0, 8), (1, 4)))
    final_gain = jnp.clip(1.0 + 0.18 * jax.random.normal(seeds[15], (D,), jnp.float32), 0.1, 1.9)
    return {"tokens": tokens, "lengths": lengths, "state_block": state_block, "cached_keys": cached_keys, "cached_values": cached_values, "query_weight": query_weight, "key_weight": key_weight, "value_weight": value_weight, "gate_weight": gate_weight, "decay_rate": decay_rate, "head_gain": head_gain, "out_weight": out_weight, "mixer_gain": mixer_gain, "up_weight": up_weight, "down_weight": down_weight, "final_gain": final_gain}


ALPHA = 2.0 ** 0.5
EPS = 1e-05

def rotate(vectors, positions):
    half = vectors.shape[-1] // 2
    inverse = 10000.0 ** (-jnp.arange(half, dtype=jnp.float32) / half)
    angle = positions.astype(jnp.float32)[:, None] * inverse[None, :]
    cosine = jnp.cos(angle)[:, None, :]
    sine = jnp.sin(angle)[:, None, :]
    former, latter = (vectors[..., :half], vectors[..., half:])
    return jnp.concatenate([former * cosine - latter * sine, latter * cosine + former * sine], -1)

def layer_norm(values, gain):
    mean = lax.optimization_barrier(jnp.mean(values, 1, keepdims=True))
    centred = values - mean
    spread = lax.optimization_barrier(jnp.mean(centred * centred, 1, keepdims=True))
    return centred * lax.rsqrt(spread + EPS) * gain[None, :]

def retain(query, keyed, valued, gated, lengths, state, keys, values, rate, gain):
    count = query.shape[0]
    heads = rate.shape[0]
    q_rot = rotate(query.astype(jnp.float32).reshape(count, heads, HDIM), lengths).astype(jnp.bfloat16)
    k_rot = (rotate(keyed.astype(jnp.float32).reshape(count, heads, HDIM), lengths) * 0.125).astype(jnp.bfloat16)
    v_new = valued.astype(jnp.float32).reshape(count, heads, HDIM)
    cached_k = keys.astype(jnp.float32).reshape(count, BLK, heads, HDIM)
    cached_v = values.astype(jnp.float32).reshape(count, BLK, heads, HDIM)
    q_wide = q_rot.astype(jnp.float32)
    scores = jnp.einsum('shn,sihn->shi', q_wide, cached_k)
    offset = lengths % BLK
    slots = jnp.arange(BLK, dtype=jnp.int32)
    lag = jnp.maximum(offset[:, None] - slots[None, :], 0).astype(jnp.float32)
    live = (slots[None, :] < offset[:, None])[:, None, :]
    factor = jnp.where(live, jnp.exp(-rate[None, :, None] * lag[:, None, :]), 0.0)
    weights = (scores * factor).astype(jnp.bfloat16).astype(jnp.float32)
    own = lax.optimization_barrier(jnp.sum(q_wide * k_rot.astype(jnp.float32), -1)).astype(jnp.bfloat16).astype(jnp.float32)
    inner = jnp.einsum('shi,sihn->shn', weights, cached_v) + own[..., None] * v_new
    carried = jnp.exp(-rate[None, :] * (offset[:, None] + 1).astype(jnp.float32))
    cross = jnp.einsum('shk,skhv->shv', q_wide, state.reshape(count, HDIM, heads, HDIM), precision=lax.Precision.HIGHEST) * carried[..., None]
    retained = inner + cross
    mean = lax.optimization_barrier(jnp.mean(retained, -1, keepdims=True))
    centred = retained - mean
    spread = lax.optimization_barrier(jnp.mean(centred * centred, -1, keepdims=True))
    normed = centred * lax.rsqrt(spread + EPS) * gain.reshape(heads, HDIM)[None]
    gate_f = jax.nn.silu(gated.astype(jnp.float32).reshape(count, heads, HDIM))
    return (gate_f * normed).reshape(count, heads * HDIM).astype(jnp.bfloat16)

def reference(tokens, lengths, state_block, cached_keys, cached_values, query_weight, key_weight, value_weight, gate_weight, decay_rate, head_gain, out_weight, mixer_gain, up_weight, down_weight, final_gain):
    projected = [jnp.dot(tokens, weight, preferred_element_type=jnp.float32).astype(jnp.bfloat16) for weight in (query_weight, key_weight, value_weight, gate_weight)]
    blocks = ROWS // SEQ_DEV

    def split_rows(array):
        return array.reshape((blocks, SEQ_DEV) + array.shape[1:])

    def one_block(items):
        query, keyed, valued, gated, length_rows, state, keys, values = items
        return retain(query, keyed, valued, gated, length_rows, state, keys, values, decay_rate, head_gain)
    mixed = lax.map(one_block, tuple((split_rows(array) for array in projected + [lengths, state_block, cached_keys, cached_values])))
    mixed = mixed.reshape(ROWS, RW)
    branch = jnp.dot(mixed, out_weight, preferred_element_type=jnp.float32)
    hidden = layer_norm(ALPHA * tokens.astype(jnp.float32) + branch, mixer_gain).astype(jnp.bfloat16)
    upward = jnp.dot(hidden, up_weight, preferred_element_type=jnp.float32)
    active = jnp.square(jax.nn.relu(upward)).astype(jnp.bfloat16)
    downward = jnp.dot(active, down_weight, preferred_element_type=jnp.float32)
    return layer_norm(ALPHA * hidden.astype(jnp.float32) + downward, final_gain).astype(jnp.bfloat16)
```

```python
import jax
import jax.numpy as jnp
from jax import lax
from jax.experimental import pallas as pl
from jax.experimental.pallas import tpu as pltpu
from jax.sharding import PartitionSpec as P

HDIM = 64
BLK = 128
TILE = 256

ALPHA = 2.0**0.5
EPS = 1e-05
MESH = pl.DeviceIdType.MESH
F32 = jnp.float32
BF16 = jnp.bfloat16


def peer_of(axis, step):
    size = lax.axis_size(axis)
    return lax.rem(lax.axis_index(axis) + step, size)


def enter(axes):
    barrier = pltpu.get_barrier_semaphore()
    total = 0
    for axis in axes:
        for step in range(1, lax.axis_size(axis)):
            pl.semaphore_signal(
                barrier, inc=1, device_id={axis: peer_of(axis, step)}, device_id_type=MESH
            )
            total += 1
    pl.semaphore_wait(barrier, total)


def remote(axis, step, src, dst, sems, index):
    return pltpu.make_async_remote_copy(
        src_ref=src,
        dst_ref=dst,
        send_sem=sems.at[(0, *index, step - 1)],
        recv_sem=sems.at[(1, *index, step - 1)],
        device_id={axis: peer_of(axis, step)},
        device_id_type=MESH,
    )


class Gather:
    def __init__(self, axis, src, held, sems, index=()):
        me = lax.axis_index(axis)
        self.copies = [
            remote(axis, step, src, held.at[me], sems, index)
            for step in range(1, lax.axis_size(axis))
        ]

    def start(self):
        for copy in self.copies:
            copy.start()

    def wait_recv(self):
        for copy in self.copies:
            copy.wait_recv()

    def wait_send(self):
        for copy in self.copies:
            copy.wait_send()


class Scatter(Gather):
    def __init__(self, axis, parts, landed, sems, index=()):
        self.copies = [
            remote(axis, step, parts.at[peer_of(axis, step)], landed.at[step - 1], sems, index)
            for step in range(1, lax.axis_size(axis))
        ]
        self.own = parts.at[lax.axis_index(axis)]
        self.landed = landed

    def total(self):
        return self.own[...].astype(F32) + jnp.sum(self.landed[...].astype(F32), 0)


def project_kernel(tokens, *refs):
    weights, (out, rows, held, parts, landed, tok_sems, part_sems, load_sems) = refs[:4], refs[4:]
    loads = [
        pltpu.make_async_copy(weight, held.at[index], load_sems.at[index])
        for index, weight in enumerate(weights)
    ]
    for load in loads:
        load.start()
    enter(("tp", "kv"))
    gather = Gather("tp", tokens, rows, tok_sems)
    gather.start()
    rows[lax.axis_index("tp")] = tokens[...]
    gather.wait_recv()
    count, block, depth = rows.shape
    width = held.shape[2]
    seqs = parts.shape[2]
    sends = []
    for index in range(4):
        loads[index].wait()
        part = jnp.dot(
            rows[...].reshape(count * block, depth), held[index], preferred_element_type=F32
        )
        parts[index] = part.astype(BF16).reshape(-1, seqs, width)
        send = Scatter("kv", parts.at[index], landed.at[index], part_sems, (index,))
        send.start()
        sends.append(send)
    for index, send in enumerate(sends):
        send.wait_recv()
        out[:, index * width : (index + 1) * width] = send.total().astype(BF16)
    gather.wait_send()
    for send in sends:
        send.wait_send()


def project(tokens, *weights):
    ntp, nkv = lax.axis_size("tp"), lax.axis_size("kv")
    block, depth = tokens.shape
    width = weights[0].shape[1]
    seqs = block * ntp // nkv
    return pl.pallas_call(
        project_kernel,
        name="project",
        out_shape=jax.ShapeDtypeStruct((seqs, 4 * width), BF16),
        in_specs=[pl.BlockSpec(memory_space=pltpu.VMEM)] + [pl.BlockSpec(memory_space=pl.ANY)] * 4,
        out_specs=pl.BlockSpec(memory_space=pltpu.VMEM),
        scratch_shapes=[
            pltpu.VMEM((ntp, block, depth), BF16),
            pltpu.VMEM((4, depth, width), BF16),
            pltpu.VMEM((4, nkv, seqs, width), BF16),
            pltpu.VMEM((4, nkv - 1, seqs, width), BF16),
            pltpu.SemaphoreType.DMA((2, ntp - 1)),
            pltpu.SemaphoreType.DMA((2, 4, nkv - 1)),
            pltpu.SemaphoreType.DMA((4,)),
        ],
        compiler_params=pltpu.CompilerParams(
            collective_id=0, has_side_effects=True, vmem_limit_bytes=60 * 2**20
        ),
    )(tokens, *weights)


def normalize(values, gain, mine, landed, sems):
    width = values.shape[1]
    nkv = lax.axis_size("kv")
    mean = jnp.mean(values, 1, keepdims=True)
    off = values - mean
    square = jnp.sum(off * off, 1, keepdims=True)
    lane = lax.broadcasted_iota(jnp.int32, mine.shape, 1)
    mine[...] = jnp.where(lane < 64, mean, square)
    copies = [
        remote("kv", step, mine, landed.at[step - 1], sems, ()) for step in range(1, nkv)
    ]
    for copy in copies:
        copy.start()
    for copy in copies:
        copy.wait_recv()
    others = [(landed[i, :, 0:1], landed[i, :, 64:65]) for i in range(nkv - 1)]
    means = [mean] + [pair[0] for pair in others]
    overall = sum(means) / nkv
    spread = square + sum(pair[1] for pair in others)
    spread = spread + width * sum((m - overall) * (m - overall) for m in means)
    spread = spread / (width * nkv)
    for copy in copies:
        copy.wait_send()
    return (values - overall) * lax.rsqrt(spread + EPS) * gain[...]


def mixer_kernel(
    mixed, tokens, out_w, mixer_gain, up_w, down_w, final_gain, out,
    out_v, up_v, down_v, heads, branch_parts, branch_landed, stat_mine, stat_landed,
    hidden_mine, hidden_all, up_parts, up_landed, act_mine, act_all, down_sum,
    load_sems, mix_sems, branch_sems, stat_sems, hid_sems, up_sems, act_sems, down_sems,
):
    loads = [
        pltpu.make_async_copy(src, dst, load_sems.at[index])
        for index, (src, dst) in enumerate(((out_w, out_v), (up_w, up_v), (down_w, down_v)))
    ]
    for load in loads:
        load.start()
    enter(("tp", "kv"))
    nkv, seqs, width = heads.shape
    tp, kv = lax.axis_index("tp"), lax.axis_index("kv")
    ntp, block, depth = hidden_all.shape
    gather = Gather("kv", mixed, heads, mix_sems)
    gather.start()
    heads[kv] = mixed[...]
    loads[0].wait()
    gather.wait_recv()
    part = jnp.dot(heads[...].reshape(nkv * seqs, width), out_v[...], preferred_element_type=F32)
    branch_parts[0] = part.astype(BF16).reshape(ntp, block, depth)
    branch = Scatter("tp", branch_parts.at[0], branch_landed.at[0], branch_sems)
    branch.start()
    branch.wait_recv()
    values = ALPHA * tokens[...].astype(F32) + branch.total()
    hidden = normalize(values, mixer_gain, stat_mine.at[0], stat_landed.at[0], stat_sems.at[0])
    hidden_mine[...] = hidden.astype(BF16)
    spread = Gather("tp", hidden_mine, hidden_all, hid_sems)
    spread.start()
    hidden_all[tp] = hidden_mine[...]
    loads[1].wait()
    spread.wait_recv()
    tiles, tile = up_parts.shape[0], up_parts.shape[3]

    def up_scatter(index):
        return Scatter("kv", up_parts.at[index], up_landed.at[index], up_sems.at[index])

    def act_gather(index):
        return Gather("kv", act_mine.at[index], act_all.at[index], act_sems.at[index])

    @pl.loop(0, tiles)
    def _(index):
        columns = pl.ds(pl.multiple_of(index * tile, tile), tile)
        part = jnp.dot(
            hidden_all[...].reshape(ntp * block, depth), up_v[:, columns],
            preferred_element_type=F32,
        )
        up_parts[index] = part.astype(BF16).reshape(nkv, seqs, tile)
        up_scatter(index).start()

    @pl.loop(0, tiles)
    def _(index):
        send = up_scatter(index)
        send.wait_recv()
        act_mine[index] = jnp.square(jnp.maximum(send.total(), 0.0)).astype(BF16)
        act_gather(index).start()
        act_all[index, kv] = act_mine[index]

    loads[2].wait()
    down_sum[...] = jnp.zeros_like(down_sum)

    @pl.loop(0, tiles)
    def _(index):
        act_gather(index).wait_recv()
        down_sum[...] += jnp.dot(
            act_all[index].reshape(nkv * seqs, tile),
            down_v[pl.ds(pl.multiple_of(index * tile, tile), tile), :],
            preferred_element_type=F32,
        )

    branch_parts[1] = down_sum[...].astype(BF16).reshape(ntp, block, depth)
    downward = Scatter("tp", branch_parts.at[1], branch_landed.at[1], down_sems)
    downward.start()
    downward.wait_recv()
    values = ALPHA * hidden_mine[...].astype(F32) + downward.total()
    result = normalize(values, final_gain, stat_mine.at[1], stat_landed.at[1], stat_sems.at[1])
    out[...] = result.astype(BF16)
    for group in (gather, branch, spread, downward):
        group.wait_send()

    @pl.loop(0, tiles)
    def _(index):
        up_scatter(index).wait_send()
        act_gather(index).wait_send()


def mixer(mixed, tokens, out_w, mixer_gain, up_w, down_w, final_gain):
    ntp, nkv = lax.axis_size("tp"), lax.axis_size("kv")
    seqs, width = mixed.shape
    block, depth = tokens.shape
    inner = up_w.shape[1]
    tile = min(TILE, inner)
    tiles = inner // tile
    vmem, anyw = pl.BlockSpec(memory_space=pltpu.VMEM), pl.BlockSpec(memory_space=pl.ANY)
    dma = pltpu.SemaphoreType.DMA
    return pl.pallas_call(
        mixer_kernel,
        name="mixer",
        out_shape=jax.ShapeDtypeStruct((block, depth), BF16),
        in_specs=[vmem, vmem, anyw, vmem, anyw, anyw, vmem],
        out_specs=vmem,
        scratch_shapes=[
            pltpu.VMEM((width, depth), BF16),
            pltpu.VMEM((depth, inner), BF16),
            pltpu.VMEM((inner, depth), BF16),
            pltpu.VMEM((nkv, seqs, width), BF16),
            pltpu.VMEM((2, ntp, block, depth), BF16),
            pltpu.VMEM((2, ntp - 1, block, depth), BF16),
            pltpu.VMEM((2, block, 128), F32),
            pltpu.VMEM((2, nkv - 1, block, 128), F32),
            pltpu.VMEM((block, depth), BF16),
            pltpu.VMEM((ntp, block, depth), BF16),
            pltpu.VMEM((tiles, nkv, seqs, tile), BF16),
            pltpu.VMEM((tiles, nkv - 1, seqs, tile), BF16),
            pltpu.VMEM((tiles, seqs, tile), BF16),
            pltpu.VMEM((tiles, nkv, seqs, tile), BF16),
            pltpu.VMEM((ntp * block, depth), F32),
            dma((3,)),
            dma((2, nkv - 1)),
            dma((2, ntp - 1)),
            dma((2, 2, nkv - 1)),
            dma((2, ntp - 1)),
            dma((tiles, 2, nkv - 1)),
            dma((tiles, 2, nkv - 1)),
            dma((2, ntp - 1)),
        ],
        compiler_params=pltpu.CompilerParams(
            collective_id=1, has_side_effects=True, vmem_limit_bytes=60 * 2**20
        ),
    )(mixed, tokens, out_w, mixer_gain[None, :], up_w, down_w, final_gain[None, :])


def rotate(vectors, positions):
    half = vectors.shape[-1] // 2
    inverse = 10000.0 ** (-jnp.arange(half, dtype=F32) / half)
    angle = positions.astype(F32)[:, None] * inverse[None, :]
    cosine = jnp.cos(angle)[:, None, :]
    sine = jnp.sin(angle)[:, None, :]
    former, latter = (vectors[..., :half], vectors[..., half:])
    return jnp.concatenate([former * cosine - latter * sine, latter * cosine + former * sine], -1)


def retain(query, keyed, valued, gated, lengths, state, keys, values, rate, gain):
    count, width = query.shape
    heads = rate.shape[0]
    q_rot = rotate(query.astype(F32).reshape(count, heads, HDIM), lengths).astype(BF16)
    k_rot = (rotate(keyed.astype(F32).reshape(count, heads, HDIM), lengths) * 0.125).astype(BF16)
    v_new = valued.astype(F32).reshape(count, heads, HDIM)
    owner = jnp.arange(width, dtype=jnp.int32)[None, :] // HDIM == jnp.arange(heads)[:, None]
    q_wide = jnp.where(owner[None], q_rot.reshape(count, 1, width), jnp.zeros((), BF16))
    scores = jnp.einsum("shc,sic->shi", q_wide, keys, preferred_element_type=F32)
    offset = lengths % BLK
    slots = jnp.arange(BLK, dtype=jnp.int32)
    lag = jnp.maximum(offset[:, None] - slots[None, :], 0).astype(F32)
    live = (slots[None, :] < offset[:, None])[:, None, :]
    factor = jnp.where(live, jnp.exp(-rate[None, :, None] * lag[:, None, :]), 0.0)
    weights = (scores * factor).astype(BF16)
    own = jnp.einsum("shn,shn->sh", q_rot, k_rot, preferred_element_type=F32).astype(BF16)
    inner = jnp.einsum("shi,sic->shc", weights, values, preferred_element_type=F32)
    carried = jnp.exp(-rate[None, :] * (offset[:, None] + 1).astype(F32))
    cross = jnp.einsum(
        "shk,skc->shc", q_rot, state.astype(BF16), preferred_element_type=F32
    )
    both = jnp.sum(jnp.where(owner[None], inner + cross * carried[..., None], 0.0), 1)
    retained = both.reshape(count, heads, HDIM) + own.astype(F32)[..., None] * v_new
    mean = jnp.mean(retained, -1, keepdims=True)
    centred = retained - mean
    spread = jnp.mean(centred * centred, -1, keepdims=True)
    normed = centred * lax.rsqrt(spread + EPS) * gain.reshape(heads, HDIM)[None]
    gate_f = jax.nn.silu(gated.astype(F32).reshape(count, heads, HDIM))
    return (gate_f * normed).reshape(count, heads * HDIM).astype(BF16)


def per_device(
    tokens,
    lengths,
    state_block,
    cached_keys,
    cached_values,
    query_weight,
    key_weight,
    value_weight,
    gate_weight,
    decay_rate,
    head_gain,
    out_weight,
    mixer_gain,
    up_weight,
    down_weight,
    final_gain,
):
    width = query_weight.shape[1]
    summed = project(tokens, query_weight, key_weight, value_weight, gate_weight)
    query, keyed, valued, gated = [
        summed[:, index * width : (index + 1) * width] for index in range(4)
    ]
    mixed = retain(
        query,
        keyed,
        valued,
        gated,
        lengths,
        state_block,
        cached_keys,
        cached_values,
        decay_rate,
        head_gain,
    )
    return mixer(mixed, tokens, out_weight, mixer_gain, up_weight, down_weight, final_gain)


def solution(mesh):
    return jax.shard_map(
        per_device,
        mesh=mesh,
        in_specs=(
            P("tp", "kv"),
            P("kv"),
            P("kv", None, "tp"),
            P("kv", None, "tp"),
            P("kv", None, "tp"),
            P("kv", "tp"),
            P("kv", "tp"),
            P("kv", "tp"),
            P("kv", "tp"),
            P("tp"),
            P("tp"),
            P("tp", "kv"),
            P("kv"),
            P("kv", "tp"),
            P("tp", "kv"),
            P("kv"),
        ),
        out_specs=P("tp", "kv"),
        check_vma=False,
    )
```

```python
import jax
import jax.numpy as jnp
from jax import lax
from jax.experimental import pallas as pl
from jax.experimental.pallas import tpu as pltpu
from jax.sharding import PartitionSpec as P

HDIM = 64
BLK = 128
TILE = 256

ALPHA = 2.0**0.5
EPS = 1e-05
MESH = pl.DeviceIdType.MESH
F32 = jnp.float32
BF16 = jnp.bfloat16


def peer_of(axis, step):
    size = lax.axis_size(axis)
    return lax.rem(lax.axis_index(axis) + step, size)


def enter(axes):
    barrier = pltpu.get_barrier_semaphore()
    total = 0
    for axis in axes:
        for step in range(1, lax.axis_size(axis)):
            pl.semaphore_signal(
                barrier, inc=1, device_id={axis: peer_of(axis, step)}, device_id_type=MESH
            )
            total += 1
    pl.semaphore_wait(barrier, total)


def remote(axis, step, src, dst, sems, index):
    return pltpu.make_async_remote_copy(
        src_ref=src,
        dst_ref=dst,
        send_sem=sems.at[(0, *index, step - 1)],
        recv_sem=sems.at[(1, *index, step - 1)],
        device_id={axis: peer_of(axis, step)},
        device_id_type=MESH,
    )


class Gather:
    def __init__(self, axis, src, held, sems, index=()):
        me = lax.axis_index(axis)
        self.copies = [
            remote(axis, step, src, held.at[me], sems, index)
            for step in range(1, lax.axis_size(axis))
        ]

    def start(self):
        for copy in self.copies:
            copy.start()

    def wait_recv(self):
        for copy in self.copies:
            copy.wait_recv()

    def wait_send(self):
        for copy in self.copies:
            copy.wait_send()


class Scatter(Gather):
    def __init__(self, axis, parts, landed, sems, index=()):
        self.copies = [
            remote(axis, step, parts.at[peer_of(axis, step)], landed.at[step - 1], sems, index)
            for step in range(1, lax.axis_size(axis))
        ]
        self.own = parts.at[lax.axis_index(axis)]
        self.landed = landed

    def total(self):
        return self.own[...].astype(F32) + jnp.sum(self.landed[...].astype(F32), 0)


PAIR = 2


def chip():
    me = lax.axis_index("tp")
    return me // PAIR, lax.rem(me, PAIR), lax.axis_size("tp") // PAIR


def to_tp(target, src, dst, sems, index):
    return pltpu.make_async_remote_copy(
        src_ref=src,
        dst_ref=dst,
        send_sem=sems.at[0, index],
        recv_sem=sems.at[1, index],
        device_id={"tp": target},
        device_id_type=MESH,
    )


class ChipGather:
    def __init__(self, src, held, sems):
        z, core, chips = chip()
        me, other = z * PAIR + core, z * PAIR + 1 - core
        self.first = [to_tp(other, src, held.at[me], sems, 0)]
        self.handed = []
        for step in range(1, chips):
            target = lax.rem(z + step, chips) * PAIR + core
            self.first.append(to_tp(target, src, held.at[me], sems, step))
            owner = lax.rem(z + chips - step, chips) * PAIR + core
            block = held.at[owner]
            self.handed.append(to_tp(other, block, block, sems, chips + step - 1))

    def start(self):
        for copy in self.first[1:] + self.first[:1]:
            copy.start()

    def wait_recv(self):
        for copy, handed in zip(self.first[1:], self.handed):
            copy.wait_recv()
            handed.start()
        self.first[0].wait_recv()
        for handed in self.handed:
            handed.wait_recv()

    def wait_send(self):
        for copy in self.first + self.handed:
            copy.wait_send()


class ChipScatter:
    def __init__(self, parts, from_pair, sums, landed, sems):
        z, core, chips = chip()
        other = z * PAIR + 1 - core
        self.parts, self.from_pair, self.sums, self.landed = parts, from_pair, sums, landed
        self.pair, self.far = [], []
        for step in list(range(1, chips)) + [0]:
            there = lax.rem(z + step, chips)
            self.pair.append(
                to_tp(other, parts.at[1 - core, there], from_pair.at[there], sems, step)
            )
            if step:
                self.far.append(
                    to_tp(
                        there * PAIR + core, sums.at[step - 1], landed.at[step - 1], sems,
                        chips + step - 1,
                    )
                )

    def fill(self, part):
        _, _, chips = chip()
        split = part.astype(BF16).reshape(chips, PAIR, *self.landed.shape[1:])
        for core in range(PAIR):
            self.parts[core] = split[:, core]

    def total(self):
        z, core, chips = chip()
        for copy in self.pair:
            copy.start()
        for step in range(1, chips):
            there = lax.rem(z + step, chips)
            self.pair[step - 1].wait_recv()
            both = self.parts[core, there].astype(F32) + self.from_pair[there].astype(F32)
            self.sums[step - 1] = both.astype(BF16)
            self.far[step - 1].start()
        self.pair[chips - 1].wait_recv()
        both = self.parts[core, z].astype(F32) + self.from_pair[z].astype(F32)
        for copy in self.far:
            copy.wait_recv()
        return both + jnp.sum(self.landed[...].astype(F32), 0)

    def wait_send(self):
        for copy in self.pair + self.far:
            copy.wait_send()


def project_kernel(tokens, *refs):
    weights, (out, rows, held, parts, landed, tok_sems, part_sems, load_sems) = refs[:4], refs[4:]
    loads = [
        pltpu.make_async_copy(weight, held.at[index], load_sems.at[index])
        for index, weight in enumerate(weights)
    ]
    for load in loads:
        load.start()
    enter(("tp", "kv"))
    gather = ChipGather(tokens, rows, tok_sems)
    gather.start()
    rows[lax.axis_index("tp")] = tokens[...]
    gather.wait_recv()
    count, block, depth = rows.shape
    width = held.shape[2]
    seqs = parts.shape[2]
    sends = []
    for index in range(4):
        loads[index].wait()
        part = jnp.dot(
            rows[...].reshape(count * block, depth), held[index], preferred_element_type=F32
        )
        parts[index] = part.astype(BF16).reshape(-1, seqs, width)
        send = Scatter("kv", parts.at[index], landed.at[index], part_sems, (index,))
        send.start()
        sends.append(send)
    for index, send in enumerate(sends):
        send.wait_recv()
        out[:, index * width : (index + 1) * width] = send.total().astype(BF16)
    gather.wait_send()
    for send in sends:
        send.wait_send()


def project(tokens, *weights):
    ntp, nkv = lax.axis_size("tp"), lax.axis_size("kv")
    block, depth = tokens.shape
    width = weights[0].shape[1]
    seqs = block * ntp // nkv
    return pl.pallas_call(
        project_kernel,
        name="project",
        out_shape=jax.ShapeDtypeStruct((seqs, 4 * width), BF16),
        in_specs=[pl.BlockSpec(memory_space=pltpu.VMEM)] + [pl.BlockSpec(memory_space=pl.ANY)] * 4,
        out_specs=pl.BlockSpec(memory_space=pltpu.VMEM),
        scratch_shapes=[
            pltpu.VMEM((ntp, block, depth), BF16),
            pltpu.VMEM((4, depth, width), BF16),
            pltpu.VMEM((4, nkv, seqs, width), BF16),
            pltpu.VMEM((4, nkv - 1, seqs, width), BF16),
            pltpu.SemaphoreType.DMA((2, ntp - 1)),
            pltpu.SemaphoreType.DMA((2, 4, nkv - 1)),
            pltpu.SemaphoreType.DMA((4,)),
        ],
        compiler_params=pltpu.CompilerParams(
            collective_id=0, has_side_effects=True, vmem_limit_bytes=60 * 2**20
        ),
    )(tokens, *weights)


def normalize(values, gain, mine, landed, sems):
    width = values.shape[1]
    nkv = lax.axis_size("kv")
    mean = jnp.mean(values, 1, keepdims=True)
    off = values - mean
    square = jnp.sum(off * off, 1, keepdims=True)
    lane = lax.broadcasted_iota(jnp.int32, mine.shape, 1)
    mine[...] = jnp.where(lane < 64, mean, square)
    copies = [
        remote("kv", step, mine, landed.at[step - 1], sems, ()) for step in range(1, nkv)
    ]
    for copy in copies:
        copy.start()
    for copy in copies:
        copy.wait_recv()
    others = [(landed[i, :, 0:1], landed[i, :, 64:65]) for i in range(nkv - 1)]
    means = [mean] + [pair[0] for pair in others]
    overall = sum(means) / nkv
    spread = square + sum(pair[1] for pair in others)
    spread = spread + width * sum((m - overall) * (m - overall) for m in means)
    spread = spread / (width * nkv)
    for copy in copies:
        copy.wait_send()
    return (values - overall) * lax.rsqrt(spread + EPS) * gain[...]


def mixer_kernel(
    mixed, tokens, out_w, mixer_gain, up_w, down_w, final_gain, out,
    out_v, up_v, down_v, heads, branch_parts, pair_landed, pair_sums, branch_landed, stat_mine, stat_landed,
    hidden_mine, hidden_all, up_parts, up_landed, act_mine, act_all, down_sum,
    load_sems, mix_sems, branch_sems, stat_sems, hid_sems, up_sems, act_sems, down_sems,
):
    loads = [
        pltpu.make_async_copy(src, dst, load_sems.at[index])
        for index, (src, dst) in enumerate(((out_w, out_v), (up_w, up_v), (down_w, down_v)))
    ]
    for load in loads:
        load.start()
    enter(("tp", "kv"))
    nkv, seqs, width = heads.shape
    tp, kv = lax.axis_index("tp"), lax.axis_index("kv")
    ntp, block, depth = hidden_all.shape
    gather = Gather("kv", mixed, heads, mix_sems)
    gather.start()
    heads[kv] = mixed[...]
    loads[0].wait()
    gather.wait_recv()
    part = jnp.dot(heads[...].reshape(nkv * seqs, width), out_v[...], preferred_element_type=F32)
    branch = ChipScatter(
        branch_parts.at[0], pair_landed.at[0], pair_sums.at[0], branch_landed.at[0], branch_sems
    )
    branch.fill(part)
    values = ALPHA * tokens[...].astype(F32) + branch.total()
    hidden = normalize(values, mixer_gain, stat_mine.at[0], stat_landed.at[0], stat_sems.at[0])
    hidden_mine[...] = hidden.astype(BF16)
    spread = ChipGather(hidden_mine, hidden_all, hid_sems)
    spread.start()
    hidden_all[tp] = hidden_mine[...]
    loads[1].wait()
    spread.wait_recv()
    tiles, tile = up_parts.shape[0], up_parts.shape[3]

    def up_scatter(index):
        return Scatter("kv", up_parts.at[index], up_landed.at[index], up_sems.at[index])

    def act_gather(index):
        return Gather("kv", act_mine.at[index], act_all.at[index], act_sems.at[index])

    @pl.loop(0, tiles)
    def _(index):
        columns = pl.ds(pl.multiple_of(index * tile, tile), tile)
        part = jnp.dot(
            hidden_all[...].reshape(ntp * block, depth), up_v[:, columns],
            preferred_element_type=F32,
        )
        up_parts[index] = part.astype(BF16).reshape(nkv, seqs, tile)
        up_scatter(index).start()

    @pl.loop(0, tiles)
    def _(index):
        send = up_scatter(index)
        send.wait_recv()
        act_mine[index] = jnp.square(jnp.maximum(send.total(), 0.0)).astype(BF16)
        act_gather(index).start()
        act_all[index, kv] = act_mine[index]

    loads[2].wait()
    down_sum[...] = jnp.zeros_like(down_sum)

    @pl.loop(0, tiles)
    def _(index):
        act_gather(index).wait_recv()
        down_sum[...] += jnp.dot(
            act_all[index].reshape(nkv * seqs, tile),
            down_v[pl.ds(pl.multiple_of(index * tile, tile), tile), :],
            preferred_element_type=F32,
        )

    downward = ChipScatter(
        branch_parts.at[1], pair_landed.at[1], pair_sums.at[1], branch_landed.at[1], down_sems
    )
    downward.fill(down_sum[...])
    values = ALPHA * hidden_mine[...].astype(F32) + downward.total()
    result = normalize(values, final_gain, stat_mine.at[1], stat_landed.at[1], stat_sems.at[1])
    out[...] = result.astype(BF16)
    for group in (gather, branch, spread, downward):
        group.wait_send()

    @pl.loop(0, tiles)
    def _(index):
        up_scatter(index).wait_send()
        act_gather(index).wait_send()


def mixer(mixed, tokens, out_w, mixer_gain, up_w, down_w, final_gain):
    ntp, nkv = lax.axis_size("tp"), lax.axis_size("kv")
    seqs, width = mixed.shape
    block, depth = tokens.shape
    inner = up_w.shape[1]
    chips = ntp // PAIR
    tile = min(TILE, inner)
    tiles = inner // tile
    vmem, anyw = pl.BlockSpec(memory_space=pltpu.VMEM), pl.BlockSpec(memory_space=pl.ANY)
    dma = pltpu.SemaphoreType.DMA
    return pl.pallas_call(
        mixer_kernel,
        name="mixer",
        out_shape=jax.ShapeDtypeStruct((block, depth), BF16),
        in_specs=[vmem, vmem, anyw, vmem, anyw, anyw, vmem],
        out_specs=vmem,
        scratch_shapes=[
            pltpu.VMEM((width, depth), BF16),
            pltpu.VMEM((depth, inner), BF16),
            pltpu.VMEM((inner, depth), BF16),
            pltpu.VMEM((nkv, seqs, width), BF16),
            pltpu.VMEM((2, PAIR, chips, block, depth), BF16),
            pltpu.VMEM((2, chips, block, depth), BF16),
            pltpu.VMEM((2, chips - 1, block, depth), BF16),
            pltpu.VMEM((2, chips - 1, block, depth), BF16),
            pltpu.VMEM((2, block, 128), F32),
            pltpu.VMEM((2, nkv - 1, block, 128), F32),
            pltpu.VMEM((block, depth), BF16),
            pltpu.VMEM((ntp, block, depth), BF16),
            pltpu.VMEM((tiles, nkv, seqs, tile), BF16),
            pltpu.VMEM((tiles, nkv - 1, seqs, tile), BF16),
            pltpu.VMEM((tiles, seqs, tile), BF16),
            pltpu.VMEM((tiles, nkv, seqs, tile), BF16),
            pltpu.VMEM((ntp * block, depth), F32),
            dma((3,)),
            dma((2, nkv - 1)),
            dma((2, ntp - 1)),
            dma((2, 2, nkv - 1)),
            dma((2, ntp - 1)),
            dma((tiles, 2, nkv - 1)),
            dma((tiles, 2, nkv - 1)),
            dma((2, ntp - 1)),
        ],
        compiler_params=pltpu.CompilerParams(
            collective_id=1, has_side_effects=True, vmem_limit_bytes=60 * 2**20
        ),
    )(mixed, tokens, out_w, mixer_gain[None, :], up_w, down_w, final_gain[None, :])


def rotate(vectors, positions):
    half = vectors.shape[-1] // 2
    inverse = 10000.0 ** (-jnp.arange(half, dtype=F32) / half)
    angle = positions.astype(F32)[:, None] * inverse[None, :]
    cosine = jnp.cos(angle)[:, None, :]
    sine = jnp.sin(angle)[:, None, :]
    former, latter = (vectors[..., :half], vectors[..., half:])
    return jnp.concatenate([former * cosine - latter * sine, latter * cosine + former * sine], -1)


def retain(query, keyed, valued, gated, lengths, state, keys, values, rate, gain):
    count, width = query.shape
    heads = rate.shape[0]
    q_rot = rotate(query.astype(F32).reshape(count, heads, HDIM), lengths).astype(BF16)
    k_rot = (rotate(keyed.astype(F32).reshape(count, heads, HDIM), lengths) * 0.125).astype(BF16)
    v_new = valued.astype(F32).reshape(count, heads, HDIM)
    owner = jnp.arange(width, dtype=jnp.int32)[None, :] // HDIM == jnp.arange(heads)[:, None]
    q_wide = jnp.where(owner[None], q_rot.reshape(count, 1, width), jnp.zeros((), BF16))
    scores = jnp.einsum("shc,sic->shi", q_wide, keys, preferred_element_type=F32)
    offset = lengths % BLK
    slots = jnp.arange(BLK, dtype=jnp.int32)
    lag = jnp.maximum(offset[:, None] - slots[None, :], 0).astype(F32)
    live = (slots[None, :] < offset[:, None])[:, None, :]
    factor = jnp.where(live, jnp.exp(-rate[None, :, None] * lag[:, None, :]), 0.0)
    weights = (scores * factor).astype(BF16)
    own = jnp.einsum("shn,shn->sh", q_rot, k_rot, preferred_element_type=F32).astype(BF16)
    inner = jnp.einsum("shi,sic->shc", weights, values, preferred_element_type=F32)
    carried = jnp.exp(-rate[None, :] * (offset[:, None] + 1).astype(F32))
    cross = jnp.einsum(
        "shk,skc->shc", q_rot, state.astype(BF16), preferred_element_type=F32
    )
    both = jnp.sum(jnp.where(owner[None], inner + cross * carried[..., None], 0.0), 1)
    retained = both.reshape(count, heads, HDIM) + own.astype(F32)[..., None] * v_new
    mean = jnp.mean(retained, -1, keepdims=True)
    centred = retained - mean
    spread = jnp.mean(centred * centred, -1, keepdims=True)
    normed = centred * lax.rsqrt(spread + EPS) * gain.reshape(heads, HDIM)[None]
    gate_f = jax.nn.silu(gated.astype(F32).reshape(count, heads, HDIM))
    return (gate_f * normed).reshape(count, heads * HDIM).astype(BF16)


def per_device(
    tokens,
    lengths,
    state_block,
    cached_keys,
    cached_values,
    query_weight,
    key_weight,
    value_weight,
    gate_weight,
    decay_rate,
    head_gain,
    out_weight,
    mixer_gain,
    up_weight,
    down_weight,
    final_gain,
):
    width = query_weight.shape[1]
    summed = project(tokens, query_weight, key_weight, value_weight, gate_weight)
    query, keyed, valued, gated = [
        summed[:, index * width : (index + 1) * width] for index in range(4)
    ]
    mixed = retain(
        query,
        keyed,
        valued,
        gated,
        lengths,
        state_block,
        cached_keys,
        cached_values,
        decay_rate,
        head_gain,
    )
    return mixer(mixed, tokens, out_weight, mixer_gain, up_weight, down_weight, final_gain)


def solution(mesh):
    return jax.shard_map(
        per_device,
        mesh=mesh,
        in_specs=(
            P("tp", "kv"),
            P("kv"),
            P("kv", None, "tp"),
            P("kv", None, "tp"),
            P("kv", None, "tp"),
            P("kv", "tp"),
            P("kv", "tp"),
            P("kv", "tp"),
            P("kv", "tp"),
            P("tp"),
            P("tp"),
            P("tp", "kv"),
            P("kv"),
            P("kv", "tp"),
            P("tp", "kv"),
            P("kv"),
        ),
        out_specs=P("tp", "kv"),
        check_vma=False,
    )
```

```python
import math

import jax
import jax.numpy as jnp
from jax import lax
from jax.experimental import pallas as pl
from jax.experimental.pallas import tpu as pltpu
from jax.sharding import PartitionSpec as P

HDIM = 64
BLK = 128
TILE = 256

ALPHA = 2.0**0.5
EPS = 1e-05
MESH = pl.DeviceIdType.MESH
F32 = jnp.float32
BF16 = jnp.bfloat16


def peer_of(axis, step):
    size = lax.axis_size(axis)
    return lax.rem(lax.axis_index(axis) + step, size)


def enter(axes):
    barrier = pltpu.get_barrier_semaphore()
    total = 0
    for axis in axes:
        for step in range(1, lax.axis_size(axis)):
            pl.semaphore_signal(
                barrier, inc=1, device_id={axis: peer_of(axis, step)}, device_id_type=MESH
            )
            total += 1
    pl.semaphore_wait(barrier, total)


def remote(axis, step, src, dst, sems, index):
    return pltpu.make_async_remote_copy(
        src_ref=src,
        dst_ref=dst,
        send_sem=sems.at[(0, *index, step - 1)],
        recv_sem=sems.at[(1, *index, step - 1)],
        device_id={axis: peer_of(axis, step)},
        device_id_type=MESH,
    )


class Gather:
    def __init__(self, axis, src, held, sems, index=()):
        me = lax.axis_index(axis)
        self.copies = [
            remote(axis, step, src, held.at[me], sems, index)
            for step in range(1, lax.axis_size(axis))
        ]

    def start(self):
        for copy in self.copies:
            copy.start()

    def wait_recv(self):
        for copy in self.copies:
            copy.wait_recv()

    def wait_send(self):
        for copy in self.copies:
            copy.wait_send()


class Scatter(Gather):
    def __init__(self, axis, parts, landed, sems, index=()):
        self.copies = [
            remote(axis, step, parts.at[peer_of(axis, step)], landed.at[step - 1], sems, index)
            for step in range(1, lax.axis_size(axis))
        ]
        self.own = parts.at[lax.axis_index(axis)]
        self.landed = landed

    def total(self):
        return self.own[...].astype(F32) + jnp.sum(self.landed[...].astype(F32), 0)


PAIR = 2


def chip():
    me = lax.axis_index("tp")
    return me // PAIR, lax.rem(me, PAIR), lax.axis_size("tp") // PAIR


def to_tp(target, src, dst, sems, index):
    return pltpu.make_async_remote_copy(
        src_ref=src,
        dst_ref=dst,
        send_sem=sems.at[0, index],
        recv_sem=sems.at[1, index],
        device_id={"tp": target},
        device_id_type=MESH,
    )


class ChipGather:
    def __init__(self, src, held, sems):
        z, core, chips = chip()
        me, other = z * PAIR + core, z * PAIR + 1 - core
        self.first = [to_tp(other, src, held.at[me], sems, 0)]
        self.handed = []
        for step in range(1, chips):
            target = lax.rem(z + step, chips) * PAIR + core
            self.first.append(to_tp(target, src, held.at[me], sems, step))
            owner = lax.rem(z + chips - step, chips) * PAIR + core
            block = held.at[owner]
            self.handed.append(to_tp(other, block, block, sems, chips + step - 1))

    def start(self):
        for copy in self.first[1:] + self.first[:1]:
            copy.start()

    def wait_recv(self):
        for copy, handed in zip(self.first[1:], self.handed):
            copy.wait_recv()
            handed.start()
        self.first[0].wait_recv()
        for handed in self.handed:
            handed.wait_recv()

    def wait_send(self):
        for copy in self.first + self.handed:
            copy.wait_send()


class ChipScatter:
    def __init__(self, parts, from_pair, sums, landed, sems):
        z, core, chips = chip()
        other = z * PAIR + 1 - core
        self.parts, self.from_pair, self.sums, self.landed = parts, from_pair, sums, landed
        self.pair, self.far = [], []
        for step in list(range(1, chips)) + [0]:
            there = lax.rem(z + step, chips)
            self.pair.append(
                to_tp(other, parts.at[1 - core, there], from_pair.at[there], sems, step)
            )
            if step:
                self.far.append(
                    to_tp(
                        there * PAIR + core, sums.at[step - 1], landed.at[step - 1], sems,
                        chips + step - 1,
                    )
                )

    def fill(self, part):
        _, _, chips = chip()
        split = part.astype(BF16).reshape(chips, PAIR, *self.landed.shape[1:])
        for core in range(PAIR):
            self.parts[core] = split[:, core]

    def total(self):
        z, core, chips = chip()
        for copy in self.pair:
            copy.start()
        for step in range(1, chips):
            there = lax.rem(z + step, chips)
            self.pair[step - 1].wait_recv()
            both = self.parts[core, there].astype(F32) + self.from_pair[there].astype(F32)
            self.sums[step - 1] = both.astype(BF16)
            self.far[step - 1].start()
        self.pair[chips - 1].wait_recv()
        both = self.parts[core, z].astype(F32) + self.from_pair[z].astype(F32)
        for copy in self.far:
            copy.wait_recv()
        return both + jnp.sum(self.landed[...].astype(F32), 0)

    def wait_send(self):
        for copy in self.pair + self.far:
            copy.wait_send()


def project_kernel(tokens, *refs):
    weights, (out, rows, held, parts, landed, tok_sems, part_sems, load_sems) = refs[:4], refs[4:]
    loads = [
        pltpu.make_async_copy(weight, held.at[index], load_sems.at[index])
        for index, weight in enumerate(weights)
    ]
    for load in loads:
        load.start()
    enter(("tp", "kv"))
    gather = ChipGather(tokens, rows, tok_sems)
    gather.start()
    rows[lax.axis_index("tp")] = tokens[...]
    gather.wait_recv()
    count, block, depth = rows.shape
    width = held.shape[2]
    seqs = parts.shape[2]
    sends = []
    for index in range(4):
        loads[index].wait()
        part = jnp.dot(
            rows[...].reshape(count * block, depth), held[index], preferred_element_type=F32
        )
        parts[index] = part.astype(BF16).reshape(-1, seqs, width)
        send = Scatter("kv", parts.at[index], landed.at[index], part_sems, (index,))
        send.start()
        sends.append(send)
    for index, send in enumerate(sends):
        send.wait_recv()
        out[:, index * width : (index + 1) * width] = send.total().astype(BF16)
    gather.wait_send()
    for send in sends:
        send.wait_send()


def project(tokens, *weights):
    ntp, nkv = lax.axis_size("tp"), lax.axis_size("kv")
    block, depth = tokens.shape
    width = weights[0].shape[1]
    seqs = block * ntp // nkv
    return pl.pallas_call(
        project_kernel,
        name="project",
        out_shape=jax.ShapeDtypeStruct((seqs, 4 * width), BF16),
        in_specs=[pl.BlockSpec(memory_space=pltpu.VMEM)] + [pl.BlockSpec(memory_space=pl.ANY)] * 4,
        out_specs=pl.BlockSpec(memory_space=pltpu.VMEM),
        scratch_shapes=[
            pltpu.VMEM((ntp, block, depth), BF16),
            pltpu.VMEM((4, depth, width), BF16),
            pltpu.VMEM((4, nkv, seqs, width), BF16),
            pltpu.VMEM((4, nkv - 1, seqs, width), BF16),
            pltpu.SemaphoreType.DMA((2, ntp - 1)),
            pltpu.SemaphoreType.DMA((2, 4, nkv - 1)),
            pltpu.SemaphoreType.DMA((4,)),
        ],
        compiler_params=pltpu.CompilerParams(
            collective_id=0, has_side_effects=True, vmem_limit_bytes=60 * 2**20
        ),
    )(tokens, *weights)


def normalize(values, gain, mine, landed, sems):
    width = values.shape[1]
    nkv = lax.axis_size("kv")
    mean = jnp.mean(values, 1, keepdims=True)
    off = values - mean
    square = jnp.sum(off * off, 1, keepdims=True)
    lane = lax.broadcasted_iota(jnp.int32, mine.shape, 1)
    mine[...] = jnp.where(lane < 64, mean, square)
    copies = [
        remote("kv", step, mine, landed.at[step - 1], sems, ()) for step in range(1, nkv)
    ]
    for copy in copies:
        copy.start()
    for copy in copies:
        copy.wait_recv()
    others = [(landed[i, :, 0:1], landed[i, :, 64:65]) for i in range(nkv - 1)]
    means = [mean] + [pair[0] for pair in others]
    overall = sum(means) / nkv
    spread = square + sum(pair[1] for pair in others)
    spread = spread + width * sum((m - overall) * (m - overall) for m in means)
    spread = spread / (width * nkv)
    for copy in copies:
        copy.wait_send()
    return (values - overall) * lax.rsqrt(spread + EPS) * gain[...]


def mixer_kernel(
    mixed, tokens, out_w, mixer_gain, up_w, down_w, final_gain, out,
    out_v, up_v, down_v, heads, branch_parts, pair_landed, pair_sums, branch_landed, stat_mine, stat_landed,
    hidden_mine, hidden_all, up_parts, up_landed, up_sums, up_final, act_mine, act_all, down_sum,
    load_sems, mix_sems, branch_sems, stat_sems, hid_sems, up_sems, down_sems,
):
    loads = [
        pltpu.make_async_copy(src, dst, load_sems.at[index])
        for index, (src, dst) in enumerate(((out_w, out_v), (up_w, up_v), (down_w, down_v)))
    ]
    for load in loads:
        load.start()
    enter(("tp", "kv"))
    nkv, seqs, width = heads.shape
    tp, kv = lax.axis_index("tp"), lax.axis_index("kv")
    ntp, block, depth = hidden_all.shape
    gather = Gather("kv", mixed, heads, mix_sems)
    gather.start()
    heads[kv] = mixed[...]
    loads[0].wait()
    gather.wait_recv()
    part = jnp.dot(heads[...].reshape(nkv * seqs, width), out_v[...], preferred_element_type=F32)
    branch = ChipScatter(
        branch_parts.at[0], pair_landed.at[0], pair_sums.at[0], branch_landed.at[0], branch_sems
    )
    branch.fill(part)
    values = ALPHA * tokens[...].astype(F32) + branch.total()
    hidden = normalize(values, mixer_gain, stat_mine.at[0], stat_landed.at[0], stat_sems.at[0])
    hidden_mine[...] = hidden.astype(BF16)
    spread = ChipGather(hidden_mine, hidden_all, hid_sems)
    spread.start()
    hidden_all[tp] = hidden_mine[...]
    loads[1].wait()
    spread.wait_recv()
    tiles, tile = up_parts.shape[0], up_parts.shape[4]

    side = up_parts.shape[1]
    here = (kv // side, lax.rem(kv, side))

    def neighbour(axis, step):
        there = lax.rem(here[axis] + step, side)
        target = there * side + here[1] if axis == 0 else here[0] * side + there
        return there, target

    def to_kv(target, src, dst, index, stage, step):
        return pltpu.make_async_remote_copy(
            src_ref=src,
            dst_ref=dst,
            send_sem=up_sems.at[index, 0, stage, step],
            recv_sem=up_sems.at[index, 1, stage, step],
            device_id={"kv": target},
            device_id_type=MESH,
        )

    def first_sums(index, axis):
        copies = []
        for step in range(1, side):
            there, target = neighbour(axis, step)
            copies.append(
                to_kv(target, up_parts.at[index, there], up_landed.at[index, step - 1], index, 0, step)
            )
        return copies

    def second_sums(index, axis):
        copies = []
        for step in range(1, side):
            there, target = neighbour(1 - axis, step)
            copies.append(
                to_kv(target, up_sums.at[index, there], up_final.at[index, step - 1], index, 1, step)
            )
        return copies

    def first_spread(index, axis):
        return [
            to_kv(neighbour(1 - axis, step)[1], act_mine.at[index], act_all.at[index, kv], index, 2, step)
            for step in range(1, side)
        ]

    def second_spread(index, axis):
        copies = []
        for far in range(side):
            line = lax.rem(here[1 - axis] + side - far, side)
            owner = line * side + here[1] if axis == 1 else here[0] * side + line
            block = act_all.at[index, owner] if far else act_mine.at[index]
            for step in range(1, side):
                target = neighbour(axis, step)[1]
                copies.append(
                    to_kv(target, block, act_all.at[index, owner], index, 3 + far, step)
                )
        return copies

    def each_tile(body):
        @pl.loop(0, tiles // 2)
        def _(half):
            for axis in (1, 0):
                body(2 * half + (1 - axis), axis)

    def start(copies):
        for copy in copies:
            copy.start()

    def arrive(copies):
        for copy in copies:
            copy.wait_recv()

    def multiply_up(index, axis):
        columns = pl.ds(pl.multiple_of(index * tile, tile), tile)
        part = jnp.dot(
            hidden_all[...].reshape(ntp * block, depth), up_v[:, columns],
            preferred_element_type=F32,
        )
        part = part.astype(BF16).reshape(side, side, seqs, tile)
        if axis == 0:
            up_parts[index] = part
        else:
            for column in range(side):
                up_parts[index, column] = part[:, column]
        start(first_sums(index, axis))

    def add_first(index, axis):
        arrive(first_sums(index, axis))
        both = up_parts[index, here[axis]].astype(F32)
        both = both + jnp.sum(up_landed[index].astype(F32), 0)
        up_sums[index] = both.astype(BF16)
        start(second_sums(index, axis))

    def add_second(index, axis):
        arrive(second_sums(index, axis))
        both = up_sums[index, here[1 - axis]].astype(F32)
        both = both + jnp.sum(up_final[index].astype(F32), 0)
        act_mine[index] = jnp.square(jnp.maximum(both, 0.0)).astype(BF16)
        start(first_spread(index, axis))
        start(second_spread(index, axis)[: side - 1])
        act_all[index, kv] = act_mine[index]

    def hand_on(index, axis):
        arrive(first_spread(index, axis))
        start(second_spread(index, axis)[side - 1 :])

    loads[2].wait()
    down_sum[...] = jnp.zeros_like(down_sum)

    def multiply_down(index, axis):
        arrive(second_spread(index, axis))
        down_sum[...] += jnp.dot(
            act_all[index].reshape(nkv * seqs, tile),
            down_v[pl.ds(pl.multiple_of(index * tile, tile), tile), :],
            preferred_element_type=F32,
        )

    for body in (multiply_up, add_first, add_second, hand_on, multiply_down):
        each_tile(body)

    downward = ChipScatter(
        branch_parts.at[1], pair_landed.at[1], pair_sums.at[1], branch_landed.at[1], down_sems
    )
    downward.fill(down_sum[...])
    values = ALPHA * hidden_mine[...].astype(F32) + downward.total()
    result = normalize(values, final_gain, stat_mine.at[1], stat_landed.at[1], stat_sems.at[1])
    out[...] = result.astype(BF16)
    for group in (gather, branch, spread, downward):
        group.wait_send()

    def wait_sends(index, axis):
        for group in (first_sums, second_sums, first_spread, second_spread):
            for copy in group(index, axis):
                copy.wait_send()

    each_tile(wait_sends)


def mixer(mixed, tokens, out_w, mixer_gain, up_w, down_w, final_gain):
    ntp, nkv = lax.axis_size("tp"), lax.axis_size("kv")
    seqs, width = mixed.shape
    block, depth = tokens.shape
    inner = up_w.shape[1]
    chips = ntp // PAIR
    side = math.isqrt(nkv)
    tile = min(TILE, inner)
    tiles = inner // tile
    vmem, anyw = pl.BlockSpec(memory_space=pltpu.VMEM), pl.BlockSpec(memory_space=pl.ANY)
    dma = pltpu.SemaphoreType.DMA
    return pl.pallas_call(
        mixer_kernel,
        name="mixer",
        out_shape=jax.ShapeDtypeStruct((block, depth), BF16),
        in_specs=[vmem, vmem, anyw, vmem, anyw, anyw, vmem],
        out_specs=vmem,
        scratch_shapes=[
            pltpu.VMEM((width, depth), BF16),
            pltpu.VMEM((depth, inner), BF16),
            pltpu.VMEM((inner, depth), BF16),
            pltpu.VMEM((nkv, seqs, width), BF16),
            pltpu.VMEM((2, PAIR, chips, block, depth), BF16),
            pltpu.VMEM((2, chips, block, depth), BF16),
            pltpu.VMEM((2, chips - 1, block, depth), BF16),
            pltpu.VMEM((2, chips - 1, block, depth), BF16),
            pltpu.VMEM((2, block, 128), F32),
            pltpu.VMEM((2, nkv - 1, block, 128), F32),
            pltpu.VMEM((block, depth), BF16),
            pltpu.VMEM((ntp, block, depth), BF16),
            pltpu.VMEM((tiles, side, side, seqs, tile), BF16),
            pltpu.VMEM((tiles, side - 1, side, seqs, tile), BF16),
            pltpu.VMEM((tiles, side, seqs, tile), BF16),
            pltpu.VMEM((tiles, side - 1, seqs, tile), BF16),
            pltpu.VMEM((tiles, seqs, tile), BF16),
            pltpu.VMEM((tiles, nkv, seqs, tile), BF16),
            pltpu.VMEM((ntp * block, depth), F32),
            dma((3,)),
            dma((2, nkv - 1)),
            dma((2, ntp - 1)),
            dma((2, 2, nkv - 1)),
            dma((2, ntp - 1)),
            dma((tiles, 2, side + 3, side)),
            dma((2, ntp - 1)),
        ],
        compiler_params=pltpu.CompilerParams(
            collective_id=1, has_side_effects=True, vmem_limit_bytes=60 * 2**20
        ),
    )(mixed, tokens, out_w, mixer_gain[None, :], up_w, down_w, final_gain[None, :])


def rotate(vectors, positions):
    half = vectors.shape[-1] // 2
    inverse = 10000.0 ** (-jnp.arange(half, dtype=F32) / half)
    angle = positions.astype(F32)[:, None] * inverse[None, :]
    cosine = jnp.cos(angle)[:, None, :]
    sine = jnp.sin(angle)[:, None, :]
    former, latter = (vectors[..., :half], vectors[..., half:])
    return jnp.concatenate([former * cosine - latter * sine, latter * cosine + former * sine], -1)


def retain(query, keyed, valued, gated, lengths, state, keys, values, rate, gain):
    count, width = query.shape
    heads = rate.shape[0]
    q_rot = rotate(query.astype(F32).reshape(count, heads, HDIM), lengths).astype(BF16)
    k_rot = (rotate(keyed.astype(F32).reshape(count, heads, HDIM), lengths) * 0.125).astype(BF16)
    v_new = valued.astype(F32).reshape(count, heads, HDIM)
    owner = jnp.arange(width, dtype=jnp.int32)[None, :] // HDIM == jnp.arange(heads)[:, None]
    q_wide = jnp.where(owner[None], q_rot.reshape(count, 1, width), jnp.zeros((), BF16))
    scores = jnp.einsum("shc,sic->shi", q_wide, keys, preferred_element_type=F32)
    offset = lengths % BLK
    slots = jnp.arange(BLK, dtype=jnp.int32)
    lag = jnp.maximum(offset[:, None] - slots[None, :], 0).astype(F32)
    live = (slots[None, :] < offset[:, None])[:, None, :]
    factor = jnp.where(live, jnp.exp(-rate[None, :, None] * lag[:, None, :]), 0.0)
    weights = (scores * factor).astype(BF16)
    own = jnp.einsum("shn,shn->sh", q_rot, k_rot, preferred_element_type=F32).astype(BF16)
    inner = jnp.einsum("shi,sic->shc", weights, values, preferred_element_type=F32)
    carried = jnp.exp(-rate[None, :] * (offset[:, None] + 1).astype(F32))
    cross = jnp.einsum(
        "shk,skc->shc", q_rot, state.astype(BF16), preferred_element_type=F32
    )
    both = jnp.sum(jnp.where(owner[None], inner + cross * carried[..., None], 0.0), 1)
    retained = both.reshape(count, heads, HDIM) + own.astype(F32)[..., None] * v_new
    mean = jnp.mean(retained, -1, keepdims=True)
    centred = retained - mean
    spread = jnp.mean(centred * centred, -1, keepdims=True)
    normed = centred * lax.rsqrt(spread + EPS) * gain.reshape(heads, HDIM)[None]
    gate_f = jax.nn.silu(gated.astype(F32).reshape(count, heads, HDIM))
    return (gate_f * normed).reshape(count, heads * HDIM).astype(BF16)


def per_device(
    tokens,
    lengths,
    state_block,
    cached_keys,
    cached_values,
    query_weight,
    key_weight,
    value_weight,
    gate_weight,
    decay_rate,
    head_gain,
    out_weight,
    mixer_gain,
    up_weight,
    down_weight,
    final_gain,
):
    width = query_weight.shape[1]
    summed = project(tokens, query_weight, key_weight, value_weight, gate_weight)
    query, keyed, valued, gated = [
        summed[:, index * width : (index + 1) * width] for index in range(4)
    ]
    mixed = retain(
        query,
        keyed,
        valued,
        gated,
        lengths,
        state_block,
        cached_keys,
        cached_values,
        decay_rate,
        head_gain,
    )
    return mixer(mixed, tokens, out_weight, mixer_gain, up_weight, down_weight, final_gain)


def solution(mesh):
    return jax.shard_map(
        per_device,
        mesh=mesh,
        in_specs=(
            P("tp", "kv"),
            P("kv"),
            P("kv", None, "tp"),
            P("kv", None, "tp"),
            P("kv", None, "tp"),
            P("kv", "tp"),
            P("kv", "tp"),
            P("kv", "tp"),
            P("kv", "tp"),
            P("tp"),
            P("tp"),
            P("tp", "kv"),
            P("kv"),
            P("kv", "tp"),
            P("tp", "kv"),
            P("kv"),
        ),
        out_specs=P("tp", "kv"),
        check_vma=False,
    )
```

```python
import math

import jax
import jax.numpy as jnp
from jax import lax
from jax.experimental import pallas as pl
from jax.experimental.pallas import tpu as pltpu
from jax.sharding import PartitionSpec as P

HDIM = 64
BLK = 128
TILE = 256
HEAD_ROWS = 16

ALPHA = 2.0**0.5
EPS = 1e-05
MESH = pl.DeviceIdType.MESH
F32 = jnp.float32
BF16 = jnp.bfloat16


def peer_of(axis, step):
    size = lax.axis_size(axis)
    return lax.rem(lax.axis_index(axis) + step, size)


def enter(axes):
    barrier = pltpu.get_barrier_semaphore()
    total = 0
    for axis in axes:
        for step in range(1, lax.axis_size(axis)):
            pl.semaphore_signal(
                barrier, inc=1, device_id={axis: peer_of(axis, step)}, device_id_type=MESH
            )
            total += 1
    pl.semaphore_wait(barrier, total)


def remote(axis, step, src, dst, sems, index):
    return pltpu.make_async_remote_copy(
        src_ref=src,
        dst_ref=dst,
        send_sem=sems.at[(0, *index, step - 1)],
        recv_sem=sems.at[(1, *index, step - 1)],
        device_id={axis: peer_of(axis, step)},
        device_id_type=MESH,
    )


class Gather:
    def __init__(self, axis, src, held, sems, index=()):
        me = lax.axis_index(axis)
        self.copies = [
            remote(axis, step, src, held.at[me], sems, index)
            for step in range(1, lax.axis_size(axis))
        ]

    def start(self):
        for copy in self.copies:
            copy.start()

    def wait_recv(self):
        for copy in self.copies:
            copy.wait_recv()

    def wait_send(self):
        for copy in self.copies:
            copy.wait_send()


class Scatter(Gather):
    def __init__(self, axis, parts, landed, sems, index=()):
        self.copies = [
            remote(axis, step, parts.at[peer_of(axis, step)], landed.at[step - 1], sems, index)
            for step in range(1, lax.axis_size(axis))
        ]
        self.own = parts.at[lax.axis_index(axis)]
        self.landed = landed

    def total(self):
        return self.own[...].astype(F32) + jnp.sum(self.landed[...].astype(F32), 0)


PAIR = 2


def chip():
    me = lax.axis_index("tp")
    return me // PAIR, lax.rem(me, PAIR), lax.axis_size("tp") // PAIR


def to_tp(target, src, dst, sems, index):
    return pltpu.make_async_remote_copy(
        src_ref=src,
        dst_ref=dst,
        send_sem=sems.at[0, index],
        recv_sem=sems.at[1, index],
        device_id={"tp": target},
        device_id_type=MESH,
    )


class ChipGather:
    def __init__(self, src, held, sems):
        z, core, chips = chip()
        me, other = z * PAIR + core, z * PAIR + 1 - core
        self.first = [to_tp(other, src, held.at[me], sems, 0)]
        self.handed = []
        for step in range(1, chips):
            target = lax.rem(z + step, chips) * PAIR + core
            self.first.append(to_tp(target, src, held.at[me], sems, step))
            owner = lax.rem(z + chips - step, chips) * PAIR + core
            block = held.at[owner]
            self.handed.append(to_tp(other, block, block, sems, chips + step - 1))

    def start(self):
        for copy in self.first[1:] + self.first[:1]:
            copy.start()

    def wait_recv(self):
        for copy, handed in zip(self.first[1:], self.handed):
            copy.wait_recv()
            handed.start()
        self.first[0].wait_recv()
        for handed in self.handed:
            handed.wait_recv()

    def wait_send(self):
        for copy in self.first + self.handed:
            copy.wait_send()


class ChipScatter:
    def __init__(self, parts, from_pair, sums, landed, sems):
        z, core, chips = chip()
        other = z * PAIR + 1 - core
        self.parts, self.from_pair, self.sums, self.landed = parts, from_pair, sums, landed
        self.pair, self.far = [], []
        for step in list(range(1, chips)) + [0]:
            there = lax.rem(z + step, chips)
            self.pair.append(
                to_tp(other, parts.at[1 - core, there], from_pair.at[there], sems, step)
            )
            if step:
                self.far.append(
                    to_tp(
                        there * PAIR + core, sums.at[step - 1], landed.at[step - 1], sems,
                        chips + step - 1,
                    )
                )

    def fill(self, part):
        _, _, chips = chip()
        split = part.astype(BF16).reshape(chips, PAIR, *self.landed.shape[1:])
        for core in range(PAIR):
            self.parts[core] = split[:, core]

    def total(self):
        z, core, chips = chip()
        for copy in self.pair:
            copy.start()
        for step in range(1, chips):
            there = lax.rem(z + step, chips)
            self.pair[step - 1].wait_recv()
            both = self.parts[core, there].astype(F32) + self.from_pair[there].astype(F32)
            self.sums[step - 1] = both.astype(BF16)
            self.far[step - 1].start()
        self.pair[chips - 1].wait_recv()
        both = self.parts[core, z].astype(F32) + self.from_pair[z].astype(F32)
        for copy in self.far:
            copy.wait_recv()
        return both + jnp.sum(self.landed[...].astype(F32), 0)

    def wait_send(self):
        for copy in self.pair + self.far:
            copy.wait_send()


def project_kernel(caches, tokens, *refs):
    weights, (out, rows, held, parts, landed, tok_sems, part_sems, load_sems) = refs[:4], refs[4:]
    loads = [
        pltpu.make_async_copy(weight, held.at[index], load_sems.at[index])
        for index, weight in enumerate(weights)
    ]
    for load in loads:
        load.start()
    for load in caches:
        load.start()
    enter(("tp", "kv"))
    gather = ChipGather(tokens, rows, tok_sems)
    gather.start()
    rows[lax.axis_index("tp")] = tokens[...]
    gather.wait_recv()
    count, block, depth = rows.shape
    width = held.shape[2]
    seqs = parts.shape[2]
    sends = []
    for index in range(4):
        loads[index].wait()
        part = jnp.dot(
            rows[...].reshape(count * block, depth), held[index], preferred_element_type=F32
        )
        parts[index] = part.astype(BF16).reshape(-1, seqs, width)
        send = Scatter("kv", parts.at[index], landed.at[index], part_sems, (index,))
        send.start()
        sends.append(send)
    for index, send in enumerate(sends):
        send.wait_recv()
        out[:, index * width : (index + 1) * width] = send.total().astype(BF16)
    gather.wait_send()
    for send in sends:
        send.wait_send()


def load_caches(caches, held, sems):
    return [
        pltpu.make_async_copy(src, dst, sems.at[index])
        for index, (src, dst) in enumerate(zip(caches, held))
    ]


def retain_kernel(summed, cos, sin, carried, factor, gain, mixed, keys, values, state, wide, kept):
    seqs, width = mixed.shape
    rows = wide.shape[1]
    query, keyed, valued, gated = [
        summed[:, index * width : (index + 1) * width] for index in range(4)
    ]
    above = lax.broadcasted_iota(jnp.int32, (width, width), 0)
    across = lax.broadcasted_iota(jnp.int32, (width, width), 1)
    half = HDIM // 2
    first = across % HDIM < half
    swap = jnp.where(first & (above == across + half), -1.0, 0.0)
    swap = jnp.where(~first & (above == across - half), 1.0, swap).astype(BF16)
    same = jnp.where(above // HDIM == across // HDIM, 1.0, 0.0)
    tall = lax.broadcasted_iota(jnp.int32, (width, HDIM), 0)
    narrow = lax.broadcasted_iota(jnp.int32, (width, HDIM), 1)
    fold = jnp.where(tall % HDIM == narrow, 1.0, 0.0).astype(BF16)
    head = lax.broadcasted_iota(jnp.int32, (rows, width), 0)
    lane = lax.broadcasted_iota(jnp.int32, (rows, width), 1)
    owner = jnp.where(lane // HDIM == head, 1.0, 0.0)

    def rotate(vectors):
        turned = jnp.dot(vectors, swap, preferred_element_type=F32)
        return vectors.astype(F32) * cos[...] + turned * sin[...]

    def per_head(terms):
        return jnp.dot(
            terms, same, preferred_element_type=F32, precision=lax.Precision.HIGHEST
        )

    q_rot = rotate(query).astype(BF16).astype(F32)
    k_rot = (rotate(keyed) * 0.125).astype(BF16).astype(F32)
    own = per_head(q_rot * k_rot).astype(BF16).astype(F32)
    wide[...] = q_rot[:, None, :] * owner[None]
    group = 8

    @pl.loop(0, seqs // group)
    def _(outer):
        for inner in range(group):
            index = outer * group + inner
            spread = wide[index].astype(BF16)
            scores = lax.dot_general(
                spread, keys[index], (((1,), (1,)), ((), ())), preferred_element_type=F32
            )
            weights = (scores * factor[index]).astype(BF16)
            within = jnp.dot(weights, values[index], preferred_element_type=F32)
            short = jnp.dot(spread, fold, preferred_element_type=F32).astype(BF16)
            cross = jnp.dot(short, state[index].astype(BF16), preferred_element_type=F32)
            both = (within + cross * carried[pl.ds(index, 1), :]) * owner
            kept[pl.ds(index, 1), :] = jnp.sum(both, 0, keepdims=True)

    retained = kept[...] + own * valued.astype(F32)
    centred = retained - per_head(retained) * (1.0 / HDIM)
    variance = per_head(centred * centred) * (1.0 / HDIM)
    normed = centred * lax.rsqrt(variance + EPS) * gain[...]
    mixed[...] = (jax.nn.silu(gated.astype(F32)) * normed).astype(BF16)


def normalize(values, gain, mine, landed, sems):
    width = values.shape[1]
    nkv = lax.axis_size("kv")
    mean = jnp.mean(values, 1, keepdims=True)
    off = values - mean
    square = jnp.sum(off * off, 1, keepdims=True)
    lane = lax.broadcasted_iota(jnp.int32, mine.shape, 1)
    mine[...] = jnp.where(lane < 64, mean, square)
    copies = [
        remote("kv", step, mine, landed.at[step - 1], sems, ()) for step in range(1, nkv)
    ]
    for copy in copies:
        copy.start()
    for copy in copies:
        copy.wait_recv()
    others = [(landed[i, :, 0:1], landed[i, :, 64:65]) for i in range(nkv - 1)]
    means = [mean] + [pair[0] for pair in others]
    overall = sum(means) / nkv
    spread = square + sum(pair[1] for pair in others)
    spread = spread + width * sum((m - overall) * (m - overall) for m in means)
    spread = spread / (width * nkv)
    for copy in copies:
        copy.wait_send()
    return (values - overall) * lax.rsqrt(spread + EPS) * gain[...]


def mixer_kernel(
    mixed, tokens, out_w, mixer_gain, up_w, down_w, final_gain, out,
    out_v, up_v, down_v, heads, branch_parts, pair_landed, pair_sums, branch_landed, stat_mine, stat_landed,
    hidden_mine, hidden_all, up_parts, up_landed, up_sums, up_final, act_mine, act_all, down_sum,
    load_sems, mix_sems, branch_sems, stat_sems, hid_sems, up_sems, down_sems,
):
    loads = [
        pltpu.make_async_copy(src, dst, load_sems.at[index])
        for index, (src, dst) in enumerate(((out_w, out_v), (up_w, up_v), (down_w, down_v)))
    ]
    for load in loads:
        load.start()
    nkv, seqs, width = heads.shape
    tp, kv = lax.axis_index("tp"), lax.axis_index("kv")
    ntp, block, depth = hidden_all.shape
    gather = Gather("kv", mixed, heads, mix_sems)
    gather.start()
    heads[kv] = mixed[...]
    loads[0].wait()
    gather.wait_recv()
    part = jnp.dot(heads[...].reshape(nkv * seqs, width), out_v[...], preferred_element_type=F32)
    branch = ChipScatter(
        branch_parts.at[0], pair_landed.at[0], pair_sums.at[0], branch_landed.at[0], branch_sems
    )
    branch.fill(part)
    values = ALPHA * tokens[...].astype(F32) + branch.total()
    hidden = normalize(values, mixer_gain, stat_mine.at[0], stat_landed.at[0], stat_sems.at[0])
    hidden_mine[...] = hidden.astype(BF16)
    spread = ChipGather(hidden_mine, hidden_all, hid_sems)
    spread.start()
    hidden_all[tp] = hidden_mine[...]
    loads[1].wait()
    spread.wait_recv()
    tiles, tile = up_parts.shape[0], up_parts.shape[4]

    side = up_parts.shape[1]
    here = (kv // side, lax.rem(kv, side))

    def neighbour(axis, step):
        there = lax.rem(here[axis] + step, side)
        target = there * side + here[1] if axis == 0 else here[0] * side + there
        return there, target

    def to_kv(target, src, dst, index, stage, step):
        return pltpu.make_async_remote_copy(
            src_ref=src,
            dst_ref=dst,
            send_sem=up_sems.at[index, 0, stage, step],
            recv_sem=up_sems.at[index, 1, stage, step],
            device_id={"kv": target},
            device_id_type=MESH,
        )

    def first_sums(index, axis):
        copies = []
        for step in range(1, side):
            there, target = neighbour(axis, step)
            copies.append(
                to_kv(target, up_parts.at[index, there], up_landed.at[index, step - 1], index, 0, step)
            )
        return copies

    def second_sums(index, axis):
        copies = []
        for step in range(1, side):
            there, target = neighbour(1 - axis, step)
            copies.append(
                to_kv(target, up_sums.at[index, there], up_final.at[index, step - 1], index, 1, step)
            )
        return copies

    def first_spread(index, axis):
        return [
            to_kv(neighbour(1 - axis, step)[1], act_mine.at[index], act_all.at[index, kv], index, 2, step)
            for step in range(1, side)
        ]

    def second_spread(index, axis):
        copies = []
        for far in range(side):
            line = lax.rem(here[1 - axis] + side - far, side)
            owner = line * side + here[1] if axis == 1 else here[0] * side + line
            block = act_all.at[index, owner] if far else act_mine.at[index]
            for step in range(1, side):
                target = neighbour(axis, step)[1]
                copies.append(
                    to_kv(target, block, act_all.at[index, owner], index, 3 + far, step)
                )
        return copies

    def each_tile(body):
        @pl.loop(0, tiles // 2)
        def _(half):
            for axis in (1, 0):
                body(2 * half + (1 - axis), axis)

    def start(copies):
        for copy in copies:
            copy.start()

    def arrive(copies):
        for copy in copies:
            copy.wait_recv()

    def multiply_up(index, axis):
        columns = pl.ds(pl.multiple_of(index * tile, tile), tile)
        part = jnp.dot(
            hidden_all[...].reshape(ntp * block, depth), up_v[:, columns],
            preferred_element_type=F32,
        )
        part = part.astype(BF16).reshape(side, side, seqs, tile)
        if axis == 0:
            up_parts[index] = part
        else:
            for column in range(side):
                up_parts[index, column] = part[:, column]
        start(first_sums(index, axis))

    def add_first(index, axis):
        arrive(first_sums(index, axis))
        both = up_parts[index, here[axis]].astype(F32)
        both = both + jnp.sum(up_landed[index].astype(F32), 0)
        up_sums[index] = both.astype(BF16)
        start(second_sums(index, axis))

    def add_second(index, axis):
        arrive(second_sums(index, axis))
        both = up_sums[index, here[1 - axis]].astype(F32)
        both = both + jnp.sum(up_final[index].astype(F32), 0)
        act_mine[index] = jnp.square(jnp.maximum(both, 0.0)).astype(BF16)
        start(first_spread(index, axis))
        start(second_spread(index, axis)[: side - 1])
        act_all[index, kv] = act_mine[index]

    def hand_on(index, axis):
        arrive(first_spread(index, axis))
        start(second_spread(index, axis)[side - 1 :])

    loads[2].wait()
    down_sum[...] = jnp.zeros_like(down_sum)

    def multiply_down(index, axis):
        arrive(second_spread(index, axis))
        down_sum[...] += jnp.dot(
            act_all[index].reshape(nkv * seqs, tile),
            down_v[pl.ds(pl.multiple_of(index * tile, tile), tile), :],
            preferred_element_type=F32,
        )

    for body in (multiply_up, add_first, add_second, hand_on, multiply_down):
        each_tile(body)

    downward = ChipScatter(
        branch_parts.at[1], pair_landed.at[1], pair_sums.at[1], branch_landed.at[1], down_sems
    )
    downward.fill(down_sum[...])
    values = ALPHA * hidden_mine[...].astype(F32) + downward.total()
    result = normalize(values, final_gain, stat_mine.at[1], stat_landed.at[1], stat_sems.at[1])
    out[...] = result.astype(BF16)
    for group in (gather, branch, spread, downward):
        group.wait_send()

    def wait_sends(index, axis):
        for group in (first_sums, second_sums, first_spread, second_spread):
            for copy in group(index, axis):
                copy.wait_send()

    each_tile(wait_sends)


def layer_kernel(*refs):
    tokens, weights, tables, caches, mixes = refs[0], refs[1:5], refs[5:10], refs[10:13], refs[13:18]
    out, refs = refs[18], refs[19:]
    (summed, *own), refs = refs[:8], refs[8:]
    (mixed, keys, values, state, wide, kept, cache_sems), refs = refs[:7], refs[7:]
    loads = load_caches(caches, (keys, values, state), cache_sems)
    project_kernel(loads, tokens, *weights, summed, *own)
    for load in loads:
        load.wait()
    retain_kernel(summed, *tables, mixed, keys, values, state, wide, kept)
    mixer_kernel(mixed, tokens, *mixes, out, *refs)


def layer(tokens, weights, tables, caches, mixes):
    ntp, nkv = lax.axis_size("tp"), lax.axis_size("kv")
    block, depth = tokens.shape
    width = weights[0].shape[1]
    seqs = caches[0].shape[0]
    inner = mixes[2].shape[1]
    chips = ntp // PAIR
    side = math.isqrt(nkv)
    tile = min(TILE, inner)
    tiles = inner // tile
    vmem, anyw = pl.BlockSpec(memory_space=pltpu.VMEM), pl.BlockSpec(memory_space=pl.ANY)
    dma = pltpu.SemaphoreType.DMA
    return pl.pallas_call(
        layer_kernel,
        name="layer",
        out_shape=jax.ShapeDtypeStruct((block, depth), BF16),
        in_specs=[vmem] + [anyw] * 4 + [vmem] * 5 + [anyw] * 3 + [anyw, vmem, anyw, anyw, vmem],
        out_specs=vmem,
        scratch_shapes=[
            pltpu.VMEM((seqs, 4 * width), BF16),
            pltpu.VMEM((ntp, block, depth), BF16),
            pltpu.VMEM((4, depth, width), BF16),
            pltpu.VMEM((4, nkv, seqs, width), BF16),
            pltpu.VMEM((4, nkv - 1, seqs, width), BF16),
            dma((2, ntp - 1)),
            dma((2, 4, nkv - 1)),
            dma((4,)),
            pltpu.VMEM((seqs, width), BF16),
            *[pltpu.VMEM(cache.shape, cache.dtype) for cache in caches],
            pltpu.VMEM((seqs, HEAD_ROWS, width), F32),
            pltpu.VMEM((seqs, width), F32),
            dma((3,)),
            pltpu.VMEM((width, depth), BF16),
            pltpu.VMEM((depth, inner), BF16),
            pltpu.VMEM((inner, depth), BF16),
            pltpu.VMEM((nkv, seqs, width), BF16),
            pltpu.VMEM((2, PAIR, chips, block, depth), BF16),
            pltpu.VMEM((2, chips, block, depth), BF16),
            pltpu.VMEM((2, chips - 1, block, depth), BF16),
            pltpu.VMEM((2, chips - 1, block, depth), BF16),
            pltpu.VMEM((2, block, 128), F32),
            pltpu.VMEM((2, nkv - 1, block, 128), F32),
            pltpu.VMEM((block, depth), BF16),
            pltpu.VMEM((ntp, block, depth), BF16),
            pltpu.VMEM((tiles, side, side, seqs, tile), BF16),
            pltpu.VMEM((tiles, side - 1, side, seqs, tile), BF16),
            pltpu.VMEM((tiles, side, seqs, tile), BF16),
            pltpu.VMEM((tiles, side - 1, seqs, tile), BF16),
            pltpu.VMEM((tiles, seqs, tile), BF16),
            pltpu.VMEM((tiles, nkv, seqs, tile), BF16),
            pltpu.VMEM((ntp * block, depth), F32),
            dma((3,)),
            dma((2, nkv - 1)),
            dma((2, ntp - 1)),
            dma((2, 2, nkv - 1)),
            dma((2, ntp - 1)),
            dma((tiles, 2, side + 3, side)),
            dma((2, ntp - 1)),
        ],
        compiler_params=pltpu.CompilerParams(
            collective_id=0, has_side_effects=True, vmem_limit_bytes=60 * 2**20
        ),
    )(tokens, *weights, *tables, *caches, *mixes)


def tables_of(lengths, rate, gain):
    heads = rate.shape[0]
    half = HDIM // 2
    inverse = 10000.0 ** (-jnp.arange(half, dtype=F32) / half)
    angle = lengths.astype(F32)[:, None] * inverse[None, :]
    cos = jnp.tile(jnp.cos(angle), (1, 2 * heads))
    sin = jnp.tile(jnp.sin(angle), (1, 2 * heads))
    offset = lengths % BLK
    slots = jnp.arange(BLK, dtype=jnp.int32)
    lag = jnp.maximum(offset[:, None] - slots[None, :], 0).astype(F32)
    live = (slots[None, :] < offset[:, None])[:, None, :]
    padded = jnp.pad(rate, (0, HEAD_ROWS - heads))
    factor = jnp.where(live, jnp.exp(-padded[None, :, None] * lag[:, None, :]), 0.0)
    carried = jnp.exp(-jnp.repeat(rate, HDIM)[None, :] * (offset[:, None] + 1).astype(F32))
    return cos, sin, carried, factor, gain[None, :]


def per_device(
    tokens,
    lengths,
    state_block,
    cached_keys,
    cached_values,
    query_weight,
    key_weight,
    value_weight,
    gate_weight,
    decay_rate,
    head_gain,
    out_weight,
    mixer_gain,
    up_weight,
    down_weight,
    final_gain,
):
    return layer(
        tokens,
        (query_weight, key_weight, value_weight, gate_weight),
        tables_of(lengths, decay_rate, head_gain),
        (cached_keys, cached_values, state_block),
        (out_weight, mixer_gain[None, :], up_weight, down_weight, final_gain[None, :]),
    )


def solution(mesh):
    return jax.shard_map(
        per_device,
        mesh=mesh,
        in_specs=(
            P("tp", "kv"),
            P("kv"),
            P("kv", None, "tp"),
            P("kv", None, "tp"),
            P("kv", None, "tp"),
            P("kv", "tp"),
            P("kv", "tp"),
            P("kv", "tp"),
            P("kv", "tp"),
            P("tp"),
            P("tp"),
            P("tp", "kv"),
            P("kv"),
            P("kv", "tp"),
            P("tp", "kv"),
            P("kv"),
        ),
        out_specs=P("tp", "kv"),
        check_vma=False,
    )
```
